32 devices in a mesh: grp: 2 (over x), ep: 4 (over z), tp: 4 (over y, core).
Axes of the slice: x: 2, y: 2, z: 4, core: 2. Of those that a mesh axis runs over, the one named last changes fastest.
Arguments:
- token_rows: bfloat16 [4096, 2048], P(('grp', 'ep', 'tp')), parts along dimension 0, may hold values from -6 to 6
- norm_gain: float32 [2048], replicated, may hold values from 0.1 to 1.9
- norm_bias: float32 [2048], replicated, may hold values from -3 to 3
- expert_ids: int32 [4096, 2], P(('grp', 'ep', 'tp')), parts along dimension 0, may hold values from 0 to 3, as said below
- route_gates: float32 [4096, 2], P(('grp', 'ep', 'tp')), parts along dimension 0, may hold values from 0.1 to 1
- gate_weight: bfloat16 [4, 2048, 512], P('tp'), may hold values from -0.125 to 0.125
- up_weight: bfloat16 [4, 2048, 512], P('tp'), may hold values from -0.125 to 0.125
- down_weight: bfloat16 [4, 512, 2048], P('tp'), may hold values from -0.25 to 0.25
Outputs:
- combined: bfloat16 [4096, 2048], P(('grp', 'ep', 'tp')), parts along dimension 0
The draws below stay inside these ranges and needn't reach their ends.
There are 2 independent parts, one for each index of `grp`. The reference program is written for one: setup_inputs(seed, part) draws one part's arguments, and reference() takes and returns one part's arrays. A program takes and returns all parts, laid end to end along the dimension named above; an argument that names none is the same for every part. Nothing has to cross between parts.
Inputs may be any that keep to these rules, and one draw needn't show every extreme that they name: `expert_ids`: the two experts of a token are different and lie in one group: both are among 4 * g to 4 * g + 3 for some g. In the rows of one device (aligned blocks of 128 rows) no expert is named more than 64 times, and in every such block each expert of one group is named exactly 64 times; that group is the same for all blocks of a draw.
All inputs are finite; a program needn't handle non-finite values.
Results may differ from the reference program's by a relative error of at most 0.01.
Values may be sent and summed in bfloat16 or wider, within the bound.
A program may use at most 64 MiB of HBM per device.

```python
import jax
import jax.numpy as jnp
from jax import lax

D = 2048
FF = 512
GROUP_SIZE = 4
TOK_DEV = 128
EXPERTS = 4
TOKENS = 2048
N_EP = 4
N_TP = 4


def draw_expert_ids(key, part):
    experts = N_TP
    groups = experts // GROUP_SIZE
    capacity = min(4 * TOK_DEV // experts, TOK_DEV // 2)
    group_span = 2 * capacity
    slots_all = max(groups - 1, 1) * group_span
    blocks = N_EP * N_TP
    hot_group = jax.random.randint(jax.random.fold_in(key, 7), (), 0, groups, dtype=jnp.int32)

    def one_block(block_number):
        block_key = jax.random.fold_in(key, block_number + 100)
        token_order = jax.random.permutation(jax.random.fold_in(block_key, 1), TOK_DEV).astype(jnp.int32)
        shuffled = jax.random.permutation(jax.random.fold_in(block_key, 2), slots_all).astype(jnp.int32)
        rank_list = jnp.arange(TOK_DEV, dtype=jnp.int32)
        spare_slot = shuffled[jnp.clip(rank_list - group_span, 0, slots_all - 1)]
        is_hot = rank_list < group_span
        within = jnp.where(is_hot, rank_list, spare_slot % group_span)
        other_group = spare_slot // group_span
        group_id = jnp.where(is_hot, hot_group, other_group + (other_group >= hot_group).astype(jnp.int32))
        quartet = within // GROUP_SIZE
        offset = within % GROUP_SIZE
        turn_table = jax.random.randint(jax.random.fold_in(block_key, 3), (groups,), 0, GROUP_SIZE, dtype=jnp.int32)
        group_turn = turn_table[group_id]
        lead_expert = (offset + group_turn) % GROUP_SIZE
        trail_expert = (offset + 1 + quartet % (GROUP_SIZE - 1) + group_turn) % GROUP_SIZE
        flip_bits = jax.random.randint(jax.random.fold_in(block_key, 4), (TOK_DEV,), 0, 2, dtype=jnp.int32)
        first_id = jnp.where(flip_bits == 1, trail_expert, lead_expert)
        second_id = jnp.where(flip_bits == 1, lead_expert, trail_expert)
        pair_ids = jnp.stack([group_id * GROUP_SIZE + first_id, group_id * GROUP_SIZE + second_id], axis=1)
        return jnp.zeros((TOK_DEV, 2), jnp.int32).at[token_order].set(pair_ids)
    drawn = lax.map(one_block, jnp.arange(blocks, dtype=jnp.int32))
    return drawn.reshape(blocks * TOK_DEV, 2).astype(jnp.int32)


def steps_of(own_key, dims, split, least, top_value):
    def one(dim, blocks):
        draws = jax.random.uniform(jax.random.fold_in(jax.random.fold_in(own_key, 6), dim), (blocks,), jnp.float32, least / len(split), top_value / len(split))
        return jnp.repeat(jnp.exp(draws), dims[dim] // blocks).reshape((-1,) + (1,) * (len(dims) - dim - 1))

    gain = one(*split[0])
    for cut in split[1:]:
        gain = gain * one(*cut)
    return gain


def noise(stream_key, dims, scale, most, shards=(), held_as=jnp.bfloat16):
    values = scale * jax.random.normal(stream_key, dims, jnp.float32)
    if shards:
        values = values * steps_of(stream_key, dims, shards, -0.22, 0.18)
    return jnp.clip(values, -most, most).astype(held_as)


def setup_inputs(seed: int = 0, part: int = 0) -> dict:
    key_of = jax.random.split(jax.random.key(seed), 9)
    part_splits = jax.random.split(jax.random.fold_in(key_of[8], part), 9)
    token_rows = noise(part_splits[0], (TOKENS, D), 1.0, 6.0, ((0, 16),))
    norm_gain = jnp.clip(1.0 + 0.18 * jax.random.normal(key_of[1], (D,), jnp.float32), 0.1, 1.9)
    norm_bias = noise(key_of[2], (D,), 0.5, 3.0, (), jnp.float32)
    expert_ids = draw_expert_ids(jax.random.fold_in(jax.random.fold_in(key_of[8], part), 71), part)
    route_gates = jnp.clip(0.1 + 0.9 * jax.random.uniform(part_splits[4], (TOKENS, 2), jnp.float32) ** steps_of(part_splits[4], (TOKENS, 2), ((0, 16),), -0.2, 0.2), 0.1, 1.0)
    gate_weight = noise(key_of[5], (EXPERTS, D, FF), D ** -0.5, 0.125, ((0, 4),))
    up_weight = noise(key_of[6], (EXPERTS, D, FF), D ** -0.5, 0.125, ((0, 4),))
    down_weight = noise(key_of[7], (EXPERTS, FF, D), FF ** -0.5, 0.25, ((0, 4),))
    return {"token_rows": token_rows, "norm_gain": norm_gain, "norm_bias": norm_bias, "expert_ids": expert_ids, "route_gates": route_gates, "gate_weight": gate_weight, "up_weight": up_weight, "down_weight": down_weight}


EPSILON = 1e-05

def layer_norm(token_rows, gain_vec, bias_vec):
    as_float = token_rows.astype(jnp.float32)
    center = lax.optimization_barrier(jnp.mean(as_float, axis=-1, keepdims=True))
    centered = as_float - center
    variance = lax.optimization_barrier(jnp.mean(centered * centered, axis=-1, keepdims=True))
    return (centered * lax.rsqrt(variance + EPSILON) * gain_vec + bias_vec).astype(jnp.bfloat16)

def reference(token_rows, norm_gain, norm_bias, expert_ids, route_gates, gate_weight, up_weight, down_weight):
    token_count, row_width = token_rows.shape
    experts = gate_weight.shape[0]
    blocks = token_count // TOK_DEV
    capacity = min(4 * TOK_DEV // experts, TOK_DEV // 2)
    normed = layer_norm(token_rows, norm_gain, norm_bias)
    padded = jnp.concatenate([normed, jnp.zeros((1, row_width), jnp.bfloat16)], axis=0)
    block_ids = expert_ids.reshape(blocks, 2 * TOK_DEV)
    onehot = (block_ids[:, :, None] == jnp.arange(experts, dtype=jnp.int32)[None, None, :]).astype(jnp.int32)
    slot_index = lax.optimization_barrier(jnp.sum((jnp.cumsum(onehot, axis=1) - 1) * onehot, axis=2))
    block_number = jnp.arange(blocks, dtype=jnp.int32)[:, None]
    target = ((block_ids * blocks + block_number) * capacity + slot_index).reshape(-1)
    owner_row = jnp.arange(2 * token_count, dtype=jnp.int32) // 2
    row_table = jnp.full((experts * blocks * capacity,), token_count, jnp.int32).at[target].set(owner_row)
    gate_table = jnp.zeros((experts * blocks * capacity,), jnp.float32).at[target].set(route_gates.reshape(-1))
    row_table = row_table.reshape(experts, blocks * capacity)
    gate_table = gate_table.reshape(experts, blocks * capacity)

    def one_expert(summed, pieces):
        row_index, gate_matrix, up_matrix, down_matrix, row_gates = pieces
        chosen = padded[row_index]
        gate_act = jnp.dot(chosen, gate_matrix, preferred_element_type=jnp.float32)
        up_act = jnp.dot(chosen, up_matrix, preferred_element_type=jnp.float32)
        hidden = (jax.nn.silu(gate_act) * up_act).astype(jnp.bfloat16)
        output = jnp.dot(hidden, down_matrix, preferred_element_type=jnp.float32)
        weighted = (row_gates[:, None] * output).astype(jnp.bfloat16)
        summed = summed.at[row_index].add(weighted.astype(jnp.float32))
        return (summed, None)
    start = jnp.zeros((token_count + 1, row_width), jnp.float32)
    summed, _ = lax.scan(one_expert, start, (row_table, gate_weight, up_weight, down_weight, gate_table))
    return summed[:token_count].astype(jnp.bfloat16)
```

```python
import functools

import jax
import jax.numpy as jnp
from jax import lax
from jax.experimental import pallas as pl
from jax.experimental.pallas import tpu as pltpu
from jax.sharding import PartitionSpec as P

EPSILON = 1e-05
F32 = jnp.float32
BF16 = jnp.bfloat16
MESH = pl.DeviceIdType.MESH
CHUNK_ROWS = 32
NORM_ROWS = 16


def dot(a, b):
    return jnp.dot(a, b, preferred_element_type=F32)


def kernel(
    tp_count, cores, capacity, chunks,
    tokens_ref, gain_ref, bias_ref, ids_ref, gates_ref, wg_hbm, wu_hbm, wd_hbm,
    out_ref,
    wg, wu, wd, normed, near_out, near_in, near_res, near_back, far_out, far_in, far_res, far_back, total,
    w_sem, near_send, near_recv, near_rsend, near_rrecv, far_send, far_recv, far_rsend, far_rrecv,
):
    tok_count, width = tokens_ref.shape
    chips = tp_count // cores
    far = tp_count - cores
    rows = capacity // chunks
    me = lax.axis_index("tp")
    my_chip, my_core = me // cores, me % cores

    def peer(slot):
        return (my_chip + slot // cores) % chips * cores + (my_core + slot % cores) % cores

    def origin(slot):
        return (my_chip + chips - slot // cores) % chips * cores + (my_core + cores - slot % cores) % cores

    loads = [
        pltpu.make_async_copy(src.at[0], dst, w_sem.at[i])
        for i, (src, dst) in enumerate(((wg_hbm, wg), (wu_hbm, wu), (wd_hbm, wd)))
    ]
    for load in loads:
        load.start()
    barrier = pltpu.get_barrier_semaphore()
    for slot in range(1, tp_count):
        pl.semaphore_signal(barrier, inc=1, device_id={"tp": peer(slot)}, device_id_type=MESH)

    gain = gain_ref[...]
    bias = bias_ref[...]

    def norm_block(i, carry):
        at = pl.ds(pl.multiple_of(i * NORM_ROWS, NORM_ROWS), NORM_ROWS)
        x = tokens_ref[at, :].astype(F32)
        center = jnp.mean(x, axis=-1, keepdims=True)
        centered = x - center
        variance = jnp.mean(centered * centered, axis=-1, keepdims=True)
        normed[at, :] = (centered * lax.rsqrt(variance + EPSILON) * gain + bias).astype(BF16)
        return carry

    lax.fori_loop(0, tok_count // NORM_ROWS, norm_block, 0, unroll=2)

    ids = ids_ref[...]
    gates = gates_ref[...]
    lanes = 128 * pl.cdiv(tp_count, 128)
    lane = lax.broadcasted_iota(jnp.int32, (tok_count, lanes), 1)
    first = ids[:, 0:1] == lane
    second = ids[:, 1:2] == lane
    named = jnp.where(first | second, 1.0, 0.0)
    gate_of = jnp.where(first, gates[:, 0:1], 0.0) + jnp.where(second, gates[:, 1:2], 0.0)
    t_row = lax.broadcasted_iota(jnp.int32, (tok_count, tok_count), 0)
    t_col = lax.broadcasted_iota(jnp.int32, (tok_count, tok_count), 1)
    before = jnp.where(t_col < t_row, 1.0, 0.0).astype(BF16)
    rank = dot(before, named.astype(BF16))
    place = jnp.where(named > 0.5, rank, -1.0)
    place_t = place.T

    expert_of_row = lax.broadcasted_iota(jnp.int32, (lanes, tok_count), 0)

    def place_row(slot):
        return jnp.sum(jnp.where(expert_of_row == peer(slot), place_t, 0.0), axis=0, keepdims=True).astype(jnp.int32)

    def pick(slot, start, count):
        want = start + lax.broadcasted_iota(jnp.int32, (count, tok_count), 0)
        return jnp.where(place_row(slot) == want, 1.0, 0.0).astype(BF16)

    def far_copy(c, f):
        return pltpu.make_async_remote_copy(
            far_out.at[c, f], far_in.at[c, f], far_send.at[c, f], far_recv.at[c, f],
            device_id={"tp": peer(cores + f)}, device_id_type=MESH)

    def far_return(c, f):
        return pltpu.make_async_remote_copy(
            far_res.at[c, f], far_back.at[c, f], far_rsend.at[c, f], far_rrecv.at[c, f],
            device_id={"tp": origin(cores + f)}, device_id_type=MESH)

    def near_copy(s):
        return pltpu.make_async_remote_copy(
            near_out.at[s], near_in.at[s], near_send.at[s], near_recv.at[s],
            device_id={"tp": peer(s)}, device_id_type=MESH)

    def near_return(s):
        return pltpu.make_async_remote_copy(
            near_res.at[s], near_back.at[s], near_rsend.at[s], near_rrecv.at[s],
            device_id={"tp": origin(s)}, device_id_type=MESH)

    for c in range(chunks):
        picks = jnp.concatenate([pick(cores + f, c * rows, rows) for f in range(far)], axis=0)
        far_out[c] = dot(picks, normed[...]).astype(BF16).reshape(far, rows, width)
        if c == 0:
            pl.semaphore_wait(barrier, tp_count - 1)
        for f in range(far):
            far_copy(c, f).start()
    near_picks = jnp.concatenate([pick(s, 0, capacity) for s in range(cores)], axis=0)
    packed = dot(near_picks, normed[...]).astype(BF16).reshape(cores, capacity, width)
    near_in[0] = packed[0]
    for s in range(1, cores):
        near_out[s] = packed[s]
        near_copy(s).start()

    def expert(rows_in):
        gate_act = dot(rows_in, wg[...])
        up_act = dot(rows_in, wu[...])
        hidden = (gate_act / (1.0 + jnp.exp(-gate_act)) * up_act).astype(BF16)
        return dot(hidden, wd[...]).astype(BF16)

    for load in loads:
        load.wait()
    for s in range(1, cores):
        near_copy(s).wait_recv()
    results = expert(near_in[...].reshape(cores * capacity, width)).reshape(cores, capacity, width)
    near_back[0] = results[0]
    for s in range(1, cores):
        near_res[s] = results[s]
        near_return(s).start()

    def far_step(c, carry):
        for f in range(far):
            far_copy(c, f).wait_recv()
        done = expert(far_in[c].reshape(far * rows, width)).reshape(far, rows, width)
        far_res[c] = done
        for f in range(far):
            far_return(c, f).start()
        return carry

    lax.fori_loop(0, chunks, far_step, 0)

    def spread(slots, start, count):
        want = lax.broadcasted_iota(jnp.int32, (tok_count, len(slots) * count), 1)
        high = jnp.zeros(want.shape, F32)
        for i, slot in enumerate(slots):
            mine = lane == peer(slot)
            at = jnp.sum(jnp.where(mine, place, 0.0), axis=1, keepdims=True).astype(jnp.int32) - start
            gate = jnp.sum(jnp.where(mine, gate_of, 0.0), axis=1, keepdims=True)
            at = jnp.where((at >= 0) & (at < count), at + i * count, -1)
            high = high + jnp.where(at == want, gate, 0.0)
        coarse = high.astype(BF16)
        return coarse, (high - coarse.astype(F32)).astype(BF16)

    for s in range(1, cores):
        near_return(s).wait_recv()
    coarse, fine = spread(range(cores), 0, capacity)
    back = near_back[...].reshape(cores * capacity, width)
    total[...] = dot(coarse, back) + dot(fine, back)

    for c in range(chunks):
        coarse, fine = spread(range(cores, tp_count), c * rows, rows)
        for f in range(far):
            far_return(c, f).wait_recv()
        back = far_back[c].reshape(far * rows, width)
        part = total[...] + (dot(coarse, back) + dot(fine, back))
        if c + 1 < chunks:
            total[...] = part
        else:
            out_ref[...] = part.astype(BF16)
    for s in range(1, cores):
        near_copy(s).wait_send()
        near_return(s).wait_send()

    def drain(c, carry):
        for f in range(far):
            far_copy(c, f).wait_send()
            far_return(c, f).wait_send()
        return carry

    lax.fori_loop(0, chunks, drain, 0)


def shards(token_rows, norm_gain, norm_bias, expert_ids, route_gates, gate_weight, up_weight, down_weight):
    tok_count, width = token_rows.shape
    hidden = gate_weight.shape[2]
    tp_count = lax.axis_size("tp")
    capacity = min(4 * tok_count // tp_count, tok_count // 2)
    cores = 2
    far = tp_count - cores
    chunks = max(1, capacity // CHUNK_ROWS)
    rows = capacity // chunks
    vmem = pl.BlockSpec(memory_space=pltpu.VMEM)
    hbm = pl.BlockSpec(memory_space=pl.ANY)
    near = pltpu.VMEM((cores, capacity, width), BF16)
    distant = pltpu.VMEM((chunks, far, rows, width), BF16)
    near_sem = pltpu.SemaphoreType.DMA((cores,))
    far_sem = pltpu.SemaphoreType.DMA((chunks, far))
    return pl.pallas_call(
        functools.partial(kernel, tp_count, cores, capacity, chunks),
        out_shape=jax.ShapeDtypeStruct((tok_count, width), BF16),
        in_specs=[vmem] * 5 + [hbm] * 3,
        out_specs=vmem,
        scratch_shapes=[
            pltpu.VMEM((width, hidden), BF16),
            pltpu.VMEM((width, hidden), BF16),
            pltpu.VMEM((hidden, width), BF16),
            pltpu.VMEM((tok_count, width), BF16),
            near, near, near, near,
            distant, distant, distant, distant,
            pltpu.VMEM((tok_count, width), F32),
            pltpu.SemaphoreType.DMA((3,)),
            near_sem, near_sem, near_sem, near_sem,
            far_sem, far_sem, far_sem, far_sem,
        ],
        compiler_params=pltpu.CompilerParams(
            collective_id=0, has_side_effects=True, vmem_limit_bytes=60 * 1024 * 1024
        ),
    )(
        token_rows, norm_gain.reshape(1, width), norm_bias.reshape(1, width),
        expert_ids, route_gates, gate_weight, up_weight, down_weight,
    )


def solution(mesh):
    rows = P(("grp", "ep", "tp"), None)
    weight = P("tp", None, None)
    return jax.shard_map(
        shards, mesh=mesh,
        in_specs=(rows, P(), P(), rows, rows, weight, weight, weight),
        out_specs=rows, check_vma=False,
    )
```

```python
import functools

import jax
import jax.numpy as jnp
from jax import lax
from jax.experimental import pallas as pl
from jax.experimental.pallas import tpu as pltpu
from jax.sharding import PartitionSpec as P

EPSILON = 1e-05
F32 = jnp.float32
BF16 = jnp.bfloat16
MESH = pl.DeviceIdType.MESH
CHUNK_ROWS = 32
NORM_ROWS = 16
BLOCKS = 4
VMEM_BYTES = 60 * 1024 * 1024
IN_SPACE = pltpu.HBM


def dot(a, b):
    return jnp.dot(a, b, preferred_element_type=F32)


def kernel(
    tp_count, cores, capacity, chunks,
    tokens_hbm, gain_hbm, bias_hbm, ids_hbm, gates_hbm, wg_hbm, wu_hbm, wd_hbm,
    out_hbm,
    tokens, gain_ref, bias_ref, ids_ref, gates_ref, wg, wu, wd, normed,
    near_out, near_in, near_res, near_back, far_out, far_in, far_res, far_back, total, result,
    w_sem, out_sem, near_send, near_recv, near_rsend, near_rrecv, far_send, far_recv, far_rsend, far_rrecv,
):
    tok_count, width = tokens.shape
    chips = tp_count // cores
    far = tp_count - cores
    rows = capacity // chunks
    block = width // BLOCKS
    me = lax.axis_index("tp")
    my_chip, my_core = me // cores, me % cores

    def peer(slot):
        return (my_chip + slot // cores) % chips * cores + (my_core + slot % cores) % cores

    def origin(slot):
        return (my_chip + chips - slot // cores) % chips * cores + (my_core + cores - slot % cores) % cores

    barrier = pltpu.get_barrier_semaphore()
    for slot in range(1, tp_count):
        pl.semaphore_signal(barrier, inc=1, device_id={"tp": peer(slot)}, device_id_type=MESH)
    pairs = (
        (ids_hbm, ids_ref), (tokens_hbm, tokens), (gates_hbm, gates_ref), (gain_hbm, gain_ref), (bias_hbm, bias_ref),
        (wg_hbm.at[0], wg), (wu_hbm.at[0], wu), (wd_hbm.at[0], wd),
    )
    loads = [pltpu.make_async_copy(src, dst, w_sem.at[i]) for i, (src, dst) in enumerate(pairs)]
    for load in loads:
        load.start()

    lanes = 128 * pl.cdiv(tp_count, 128)
    t_row = lax.broadcasted_iota(jnp.int32, (tok_count, tok_count), 0)
    t_col = lax.broadcasted_iota(jnp.int32, (tok_count, tok_count), 1)
    before = jnp.where(t_row < t_col, 1.0, 0.0).astype(BF16)
    expert_of_row = lax.broadcasted_iota(jnp.int32, (lanes, tok_count), 0)
    loads[0].wait()
    ids = ids_ref[...]
    first = ids[0:1, :] == expert_of_row
    second = ids[1:2, :] == expert_of_row
    named = jnp.where(first | second, 1.0, 0.0)
    rank = dot(named.astype(BF16), before)
    place_t = jnp.where(named > 0.5, rank, -1.0)

    def place_row(slot):
        return jnp.sum(jnp.where(expert_of_row == peer(slot), place_t, 0.0), axis=0, keepdims=True).astype(jnp.int32)

    def pick(slot, start, count):
        want = start + lax.broadcasted_iota(jnp.int32, (count, tok_count), 0)
        return jnp.where(place_row(slot) == want, 1.0, 0.0).astype(BF16)

    def far_copy(c, f):
        return pltpu.make_async_remote_copy(
            far_out.at[c, f], far_in.at[c, f], far_send.at[c, f], far_recv.at[c, f],
            device_id={"tp": peer(cores + f)}, device_id_type=MESH)

    def far_return(c, f, j):
        at = pl.ds(j * block, block)
        return pltpu.make_async_remote_copy(
            far_res.at[c, f, :, at], far_back.at[c, f, :, at], far_rsend.at[c, f, j], far_rrecv.at[c, f, j],
            device_id={"tp": origin(cores + f)}, device_id_type=MESH)

    def near_copy(s):
        return pltpu.make_async_remote_copy(
            near_out.at[s], near_in.at[s], near_send.at[s], near_recv.at[s],
            device_id={"tp": peer(s)}, device_id_type=MESH)

    def near_return(s):
        return pltpu.make_async_remote_copy(
            near_res.at[s], near_back.at[s], near_rsend.at[s], near_rrecv.at[s],
            device_id={"tp": origin(s)}, device_id_type=MESH)

    for c in range(chunks):
        picks = jnp.concatenate([pick(cores + f, c * rows, rows) for f in range(far)], axis=0)
        if c == 0:
            loads[1].wait()
        far_out[c] = dot(picks, tokens[...]).astype(BF16).reshape(far, rows, width)
        if c == 0:
            pl.semaphore_wait(barrier, tp_count - 1)
        for f in range(far):
            far_copy(c, f).start()
    near_picks = jnp.concatenate([pick(s, 0, capacity) for s in range(cores)], axis=0)
    packed = dot(near_picks, tokens[...]).astype(BF16).reshape(cores, capacity, width)
    near_in[0] = packed[0]
    for s in range(1, cores):
        near_out[s] = packed[s]
        near_copy(s).start()

    for load in loads[2:5]:
        load.wait()
    gates = gates_ref[...]
    place = place_t.T
    gate_of = (jnp.where(first, gates[0:1, :], 0.0) + jnp.where(second, gates[1:2, :], 0.0)).T
    lane = lax.broadcasted_iota(jnp.int32, (tok_count, lanes), 1)

    def norm(load_rows, count):
        gain = gain_ref[...]
        bias = bias_ref[...]

        def norm_block(i, carry):
            at = pl.multiple_of(i * NORM_ROWS, NORM_ROWS)
            x = load_rows(at).astype(F32)
            center = jnp.mean(x, axis=-1, keepdims=True)
            centered = x - center
            variance = jnp.mean(centered * centered, axis=-1, keepdims=True)
            normed[pl.ds(at, NORM_ROWS), :] = (centered * lax.rsqrt(variance + EPSILON) * gain + bias).astype(BF16)
            return carry

        lax.fori_loop(0, count // NORM_ROWS, norm_block, 0)

    def hidden_of(count):
        rows_in = normed[pl.ds(0, count), :]
        gate_act = dot(rows_in, wg[...])
        up_act = dot(rows_in, wu[...])
        return (gate_act / (1.0 + jnp.exp(-gate_act)) * up_act).astype(BF16)

    for s in range(1, cores):
        near_copy(s).wait_recv()
    norm(lambda at: near_in[at // capacity, pl.ds(pl.multiple_of(at % capacity, NORM_ROWS), NORM_ROWS), :], cores * capacity)
    for load in loads[5:]:
        load.wait()
    results = dot(hidden_of(cores * capacity), wd[...]).astype(BF16).reshape(cores, capacity, width)
    near_back[0] = results[0]
    for s in range(1, cores):
        near_res[s] = results[s]
        near_return(s).start()

    def far_step(c, carry):
        for f in range(far):
            far_copy(c, f).wait_recv()
        norm(lambda at: far_in[c, at // rows, pl.ds(pl.multiple_of(at % rows, NORM_ROWS), NORM_ROWS), :], far * rows)
        hidden = hidden_of(far * rows)
        for j in range(BLOCKS):
            at = pl.ds(j * block, block)
            far_res[c, :, :, at] = dot(hidden, wd[:, at]).astype(BF16).reshape(far, rows, block)
            for f in range(far):
                far_return(c, f, j).start()
        return carry

    lax.fori_loop(0, chunks, far_step, 0)

    def spread(slots, start, count):
        want = lax.broadcasted_iota(jnp.int32, (tok_count, len(slots) * count), 1)
        high = jnp.zeros(want.shape, F32)
        for i, slot in enumerate(slots):
            mine = lane == peer(slot)
            at = jnp.sum(jnp.where(mine, place, 0.0), axis=1, keepdims=True).astype(jnp.int32) - start
            gate = jnp.sum(jnp.where(mine, gate_of, 0.0), axis=1, keepdims=True)
            at = jnp.where((at >= 0) & (at < count), at + i * count, -1)
            high = high + jnp.where(at == want, gate, 0.0)
        coarse = high.astype(BF16)
        return coarse, (high - coarse.astype(F32)).astype(BF16)

    for s in range(1, cores):
        near_return(s).wait_recv()
    coarse, fine = spread(range(cores), 0, capacity)
    back = near_back[...].reshape(cores * capacity, width)
    total[...] = dot(coarse, back) + dot(fine, back)

    for c in range(chunks):
        coarse, fine = spread(range(cores, tp_count), c * rows, rows)
        for j in range(BLOCKS):
            at = pl.ds(j * block, block)
            for f in range(far):
                far_return(c, f, j).wait_recv()
            back = far_back[c, :, :, at].reshape(far * rows, block)
            part = total[:, at] + (dot(coarse, back) + dot(fine, back))
            if c + 1 < chunks:
                total[:, at] = part
            else:
                result[:, at] = part.astype(BF16)
                pltpu.make_async_copy(result.at[:, at], out_hbm.at[:, at], out_sem.at[j]).start()
    for s in range(1, cores):
        near_copy(s).wait_send()
        near_return(s).wait_send()

    def drain(c, carry):
        for f in range(far):
            far_copy(c, f).wait_send()
            for j in range(BLOCKS):
                far_return(c, f, j).wait_send()
        return carry

    lax.fori_loop(0, chunks, drain, 0)
    for j in range(BLOCKS):
        at = pl.ds(j * block, block)
        pltpu.make_async_copy(result.at[:, at], out_hbm.at[:, at], out_sem.at[j]).wait()


def shards(token_rows, norm_gain, norm_bias, expert_ids, route_gates, gate_weight, up_weight, down_weight):
    tok_count, width = token_rows.shape
    hidden = gate_weight.shape[2]
    tp_count = lax.axis_size("tp")
    capacity = min(4 * tok_count // tp_count, tok_count // 2)
    cores = 2
    far = tp_count - cores
    chunks = max(1, capacity // CHUNK_ROWS)
    rows = capacity // chunks
    near = pltpu.VMEM((cores, capacity, width), BF16)
    distant = pltpu.VMEM((chunks, far, rows, width), BF16)
    near_sem = pltpu.SemaphoreType.DMA((cores,))
    far_sem = pltpu.SemaphoreType.DMA((chunks, far))
    ret_sem = pltpu.SemaphoreType.DMA((chunks, far, BLOCKS))
    return pl.pallas_call(
        functools.partial(kernel, tp_count, cores, capacity, chunks),
        out_shape=jax.ShapeDtypeStruct((tok_count, width), BF16),
        in_specs=[pl.BlockSpec(memory_space=IN_SPACE)] * 8,
        out_specs=pl.BlockSpec(memory_space=pl.ANY),
        scratch_shapes=[
            pltpu.VMEM((tok_count, width), BF16),
            pltpu.VMEM((1, width), F32),
            pltpu.VMEM((1, width), F32),
            pltpu.VMEM((2, tok_count), jnp.int32),
            pltpu.VMEM((2, tok_count), F32),
            pltpu.VMEM((width, hidden), BF16),
            pltpu.VMEM((width, hidden), BF16),
            pltpu.VMEM((hidden, width), BF16),
            pltpu.VMEM((max(cores * capacity, far * rows), width), BF16),
            near, near, near, near,
            distant, distant, distant, distant,
            pltpu.VMEM((tok_count, width), F32),
            pltpu.VMEM((tok_count, width), BF16),
            pltpu.SemaphoreType.DMA((8,)),
            pltpu.SemaphoreType.DMA((BLOCKS,)),
            near_sem, near_sem, near_sem, near_sem,
            far_sem, far_sem, ret_sem, ret_sem,
        ],
        compiler_params=pltpu.CompilerParams(
            collective_id=0, has_side_effects=True, vmem_limit_bytes=VMEM_BYTES
        ),
    )(
        token_rows, norm_gain.reshape(1, width), norm_bias.reshape(1, width),
        expert_ids.T, route_gates.T, gate_weight, up_weight, down_weight,
    )


def solution(mesh):
    rows = P(("grp", "ep", "tp"), None)
    weight = P("tp", None, None)
    return jax.shard_map(
        shards, mesh=mesh,
        in_specs=(rows, P(), P(), rows, rows, weight, weight, weight),
        out_specs=rows, check_vma=False,
    )
```

```python
import functools

import jax
import jax.numpy as jnp
from jax import lax
from jax.experimental import pallas as pl
from jax.experimental.pallas import tpu as pltpu
from jax.sharding import PartitionSpec as P

EPSILON = 1e-05
F32 = jnp.float32
BF16 = jnp.bfloat16
MESH = pl.DeviceIdType.MESH
CHUNK_ROWS = 32
NORM_ROWS = 16
BLOCKS = 2
VMEM_BYTES = 48 * 1024 * 1024
IN_SPACE = pltpu.HBM


def dot(a, b):
    return jnp.dot(a, b, preferred_element_type=F32)


def kernel(
    tp_count, cores, capacity, chunks,
    tokens_hbm, gain_hbm, bias_hbm, ids_hbm, gates_hbm, wg_hbm, wu_hbm, wd_hbm,
    out_ref,
    tokens, gain_ref, bias_ref, ids_ref, gates_ref, wg, wu, wd, normed,
    near_out, near_in, near_res, near_back, far_out, far_in, far_res, far_back, total,
    w_sem, near_send, near_recv, near_rsend, near_rrecv, far_send, far_recv, far_rsend, far_rrecv,
):
    tok_count, width = tokens.shape
    chips = tp_count // cores
    far = tp_count - cores
    rows = capacity // chunks
    block = width // BLOCKS
    me = lax.axis_index("tp")
    my_chip, my_core = me // cores, me % cores

    def peer(slot):
        return (my_chip + slot // cores) % chips * cores + (my_core + slot % cores) % cores

    def origin(slot):
        return (my_chip + chips - slot // cores) % chips * cores + (my_core + cores - slot % cores) % cores

    barrier = pltpu.get_barrier_semaphore()
    for slot in range(1, tp_count):
        pl.semaphore_signal(barrier, inc=1, device_id={"tp": peer(slot)}, device_id_type=MESH)
    pairs = (
        (ids_hbm, ids_ref), (tokens_hbm, tokens), (gates_hbm, gates_ref), (gain_hbm, gain_ref), (bias_hbm, bias_ref),
        (wg_hbm.at[0], wg), (wu_hbm.at[0], wu), (wd_hbm.at[0], wd),
    )
    loads = [pltpu.make_async_copy(src, dst, w_sem.at[i]) for i, (src, dst) in enumerate(pairs)]
    for load in loads:
        load.start()

    lanes = 128 * pl.cdiv(tp_count, 128)
    t_row = lax.broadcasted_iota(jnp.int32, (tok_count, tok_count), 0)
    t_col = lax.broadcasted_iota(jnp.int32, (tok_count, tok_count), 1)
    before = jnp.where(t_row < t_col, 1.0, 0.0).astype(BF16)
    expert_of_row = lax.broadcasted_iota(jnp.int32, (lanes, tok_count), 0)
    loads[0].wait()
    ids = ids_ref[...]
    first = ids[0:1, :] == expert_of_row
    second = ids[1:2, :] == expert_of_row
    named = jnp.where(first | second, 1.0, 0.0)
    rank = dot(named.astype(BF16), before)
    place_t = jnp.where(named > 0.5, rank, -1.0)

    def place_row(slot):
        return jnp.sum(jnp.where(expert_of_row == peer(slot), place_t, 0.0), axis=0, keepdims=True).astype(jnp.int32)

    def pick(slot, start, count):
        want = start + lax.broadcasted_iota(jnp.int32, (count, tok_count), 0)
        return jnp.where(place_row(slot) == want, 1.0, 0.0).astype(BF16)

    def far_copy(c, f):
        return pltpu.make_async_remote_copy(
            far_out.at[c, f], far_in.at[c, f], far_send.at[c, f], far_recv.at[c, f],
            device_id={"tp": peer(cores + f)}, device_id_type=MESH)

    def far_return(c, f, j):
        at = pl.ds(j * block, block)
        return pltpu.make_async_remote_copy(
            far_res.at[c, f, :, at], far_back.at[c, f, :, at], far_rsend.at[c, f, j], far_rrecv.at[c, f, j],
            device_id={"tp": origin(cores + f)}, device_id_type=MESH)

    def near_copy(s):
        return pltpu.make_async_remote_copy(
            near_out.at[s], near_in.at[s], near_send.at[s], near_recv.at[s],
            device_id={"tp": peer(s)}, device_id_type=MESH)

    def near_return(s):
        return pltpu.make_async_remote_copy(
            near_res.at[s], near_back.at[s], near_rsend.at[s], near_rrecv.at[s],
            device_id={"tp": origin(s)}, device_id_type=MESH)

    for c in range(chunks):
        picks = jnp.concatenate([pick(cores + f, c * rows, rows) for f in range(far)], axis=0)
        if c == 0:
            loads[1].wait()
        far_out[c] = dot(picks, tokens[...]).astype(BF16).reshape(far, rows, width)
        if c == 0:
            pl.semaphore_wait(barrier, tp_count - 1)
        for f in range(far):
            far_copy(c, f).start()
    near_picks = jnp.concatenate([pick(s, 0, capacity) for s in range(cores)], axis=0)
    packed = dot(near_picks, tokens[...]).astype(BF16).reshape(cores, capacity, width)
    near_in[0] = packed[0]
    for s in range(1, cores):
        near_out[s] = packed[s]
        near_copy(s).start()

    for load in loads[2:5]:
        load.wait()
    gates = gates_ref[...]
    place = place_t.T
    gate_of = (jnp.where(first, gates[0:1, :], 0.0) + jnp.where(second, gates[1:2, :], 0.0)).T
    lane = lax.broadcasted_iota(jnp.int32, (tok_count, lanes), 1)

    def norm(load_rows, count):
        gain = gain_ref[...]
        bias = bias_ref[...]

        def norm_block(i, carry):
            at = pl.multiple_of(i * NORM_ROWS, NORM_ROWS)
            x = load_rows(at).astype(F32)
            center = jnp.mean(x, axis=-1, keepdims=True)
            centered = x - center
            variance = jnp.mean(centered * centered, axis=-1, keepdims=True)
            normed[pl.ds(at, NORM_ROWS), :] = (centered * lax.rsqrt(variance + EPSILON) * gain + bias).astype(BF16)
            return carry

        lax.fori_loop(0, count // NORM_ROWS, norm_block, 0)

    def hidden_of(count):
        rows_in = normed[pl.ds(0, count), :]
        gate_act = dot(rows_in, wg[...])
        up_act = dot(rows_in, wu[...])
        return (gate_act / (1.0 + jnp.exp(-gate_act)) * up_act).astype(BF16)

    for s in range(1, cores):
        near_copy(s).wait_recv()
    norm(lambda at: near_in[at // capacity, pl.ds(pl.multiple_of(at % capacity, NORM_ROWS), NORM_ROWS), :], cores * capacity)
    for load in loads[5:]:
        load.wait()
    results = dot(hidden_of(cores * capacity), wd[...]).astype(BF16).reshape(cores, capacity, width)
    near_back[0] = results[0]
    for s in range(1, cores):
        near_res[s] = results[s]
        near_return(s).start()

    def far_step(c, carry):
        for f in range(far):
            far_copy(c, f).wait_recv()
        norm(lambda at: far_in[c, at // rows, pl.ds(pl.multiple_of(at % rows, NORM_ROWS), NORM_ROWS), :], far * rows)
        hidden = hidden_of(far * rows)
        for j in range(BLOCKS):
            at = pl.ds(j * block, block)
            far_res[c, :, :, at] = dot(hidden, wd[:, at]).astype(BF16).reshape(far, rows, block)
            for f in range(far):
                far_return(c, f, j).start()
        return carry

    lax.fori_loop(0, chunks, far_step, 0)

    def spread(slots, start, count):
        want = lax.broadcasted_iota(jnp.int32, (tok_count, len(slots) * count), 1)
        high = jnp.zeros(want.shape, F32)
        for i, slot in enumerate(slots):
            mine = lane == peer(slot)
            at = jnp.sum(jnp.where(mine, place, 0.0), axis=1, keepdims=True).astype(jnp.int32) - start
            gate = jnp.sum(jnp.where(mine, gate_of, 0.0), axis=1, keepdims=True)
            at = jnp.where((at >= 0) & (at < count), at + i * count, -1)
            high = high + jnp.where(at == want, gate, 0.0)
        coarse = high.astype(BF16)
        return coarse, (high - coarse.astype(F32)).astype(BF16)

    for s in range(1, cores):
        near_return(s).wait_recv()
    coarse, fine = spread(range(cores), 0, capacity)
    back = near_back[...].reshape(cores * capacity, width)
    total[...] = dot(coarse, back) + dot(fine, back)

    for c in range(chunks):
        coarse, fine = spread(range(cores, tp_count), c * rows, rows)
        for j in range(BLOCKS):
            at = pl.ds(j * block, block)
            for f in range(far):
                far_return(c, f, j).wait_recv()
            back = far_back[c, :, :, at].reshape(far * rows, block)
            part = total[:, at] + (dot(coarse, back) + dot(fine, back))
            if c + 1 < chunks:
                total[:, at] = part
            else:
                out_ref[:, at] = part.astype(BF16)
    for s in range(1, cores):
        near_copy(s).wait_send()
        near_return(s).wait_send()

    def drain(c, carry):
        for f in range(far):
            far_copy(c, f).wait_send()
            for j in range(BLOCKS):
                far_return(c, f, j).wait_send()
        return carry

    lax.fori_loop(0, chunks, drain, 0)


def shards(token_rows, norm_gain, norm_bias, expert_ids, route_gates, gate_weight, up_weight, down_weight):
    tok_count, width = token_rows.shape
    hidden = gate_weight.shape[2]
    tp_count = lax.axis_size("tp")
    capacity = min(4 * tok_count // tp_count, tok_count // 2)
    cores = 2
    far = tp_count - cores
    chunks = max(1, capacity // CHUNK_ROWS)
    rows = capacity // chunks
    near = pltpu.VMEM((cores, capacity, width), BF16)
    distant = pltpu.VMEM((chunks, far, rows, width), BF16)
    near_sem = pltpu.SemaphoreType.DMA((cores,))
    far_sem = pltpu.SemaphoreType.DMA((chunks, far))
    ret_sem = pltpu.SemaphoreType.DMA((chunks, far, BLOCKS))
    return pl.pallas_call(
        functools.partial(kernel, tp_count, cores, capacity, chunks),
        out_shape=pltpu.VMEM((tok_count, width), BF16),
        in_specs=[pl.BlockSpec(memory_space=IN_SPACE)] * 8,
        out_specs=pl.BlockSpec(memory_space=pltpu.VMEM),
        scratch_shapes=[
            pltpu.VMEM((tok_count, width), BF16),
            pltpu.VMEM((1, width), F32),
            pltpu.VMEM((1, width), F32),
            pltpu.VMEM((2, tok_count), jnp.int32),
            pltpu.VMEM((2, tok_count), F32),
            pltpu.VMEM((width, hidden), BF16),
            pltpu.VMEM((width, hidden), BF16),
            pltpu.VMEM((hidden, width), BF16),
            pltpu.VMEM((max(cores * capacity, far * rows), width), BF16),
            near, near, near, near,
            distant, distant, distant, distant,
            pltpu.VMEM((tok_count, width), F32),
            pltpu.SemaphoreType.DMA((8,)),
            near_sem, near_sem, near_sem, near_sem,
            far_sem, far_sem, ret_sem, ret_sem,
        ],
        compiler_params=pltpu.CompilerParams(
            collective_id=0, has_side_effects=True, vmem_limit_bytes=VMEM_BYTES
        ),
    )(
        *(pltpu.with_memory_space_constraint(x, pltpu.HBM) for x in (
            token_rows, norm_gain.reshape(1, width), norm_bias.reshape(1, width),
            expert_ids.T, route_gates.T, gate_weight, up_weight, down_weight,
        ))
    )


def solution(mesh):
    rows = P(("grp", "ep", "tp"), None)
    weight = P("tp", None, None)
    return jax.shard_map(
        shards, mesh=mesh,
        in_specs=(rows, P(), P(), rows, rows, weight, weight, weight),
        out_specs=rows, check_vma=False,
    )
```

```python
import functools

import jax
import jax.numpy as jnp
from jax import lax
from jax.experimental import pallas as pl
from jax.experimental.pallas import tpu as pltpu
from jax.sharding import PartitionSpec as P

EPSILON = 1e-05
F32 = jnp.float32
BF16 = jnp.bfloat16
MESH = pl.DeviceIdType.MESH
CHUNK_ROWS = 32
NORM_ROWS = 16
BLOCKS = 1
VMEM_BYTES = 48 * 1024 * 1024
IN_SPACE = pltpu.HBM


def dot(a, b):
    return jnp.dot(a, b, preferred_element_type=F32)


def kernel(
    tp_count, cores, capacity, chunks,
    tokens_hbm, gain_hbm, bias_hbm, ids_hbm, gates_hbm, wg_hbm, wu_hbm, wd_hbm,
    out_ref,
    tokens, gain_ref, bias_ref, ids_ref, gates_ref, wg, wu, wd, normed,
    near_out, near_in, near_res, near_back, far_out, far_in, far_res, far_back, total,
    w_sem, near_send, near_recv, near_rsend, near_rrecv, far_send, far_recv, far_rsend, far_rrecv,
):
    tok_count, width = tokens.shape
    chips = tp_count // cores
    far = tp_count - cores
    rows = capacity // chunks
    block = width // BLOCKS
    me = lax.axis_index("tp")
    my_chip, my_core = me // cores, me % cores

    def peer(slot):
        return (my_chip + slot // cores) % chips * cores + (my_core + slot % cores) % cores

    def origin(slot):
        return (my_chip + chips - slot // cores) % chips * cores + (my_core + cores - slot % cores) % cores

    barrier = pltpu.get_barrier_semaphore()
    for slot in range(1, tp_count):
        pl.semaphore_signal(barrier, inc=1, device_id={"tp": peer(slot)}, device_id_type=MESH)
    pairs = (
        (ids_hbm, ids_ref), (tokens_hbm, tokens), (gates_hbm, gates_ref), (gain_hbm, gain_ref), (bias_hbm, bias_ref),
        (wg_hbm.at[0], wg), (wu_hbm.at[0], wu), (wd_hbm.at[0], wd),
    )
    loads = [pltpu.make_async_copy(src, dst, w_sem.at[i]) for i, (src, dst) in enumerate(pairs)]
    for load in loads:
        load.start()

    lanes = 128 * pl.cdiv(tp_count, 128)
    t_row = lax.broadcasted_iota(jnp.int32, (tok_count, tok_count), 0)
    t_col = lax.broadcasted_iota(jnp.int32, (tok_count, tok_count), 1)
    before = jnp.where(t_row < t_col, 1.0, 0.0).astype(BF16)
    expert_of_row = lax.broadcasted_iota(jnp.int32, (lanes, tok_count), 0)
    loads[0].wait()
    ids = ids_ref[...]
    first = ids[0:1, :] == expert_of_row
    second = ids[1:2, :] == expert_of_row
    named = jnp.where(first | second, 1.0, 0.0)
    rank = dot(named.astype(BF16), before)
    place_t = jnp.where(named > 0.5, rank, -1.0)

    def place_row(slot):
        return jnp.sum(jnp.where(expert_of_row == peer(slot), place_t, 0.0), axis=0, keepdims=True).astype(jnp.int32)

    def pick(slot, start, count):
        want = start + lax.broadcasted_iota(jnp.int32, (count, tok_count), 0)
        return jnp.where(place_row(slot) == want, 1.0, 0.0).astype(BF16)

    def far_copy(c, f):
        return pltpu.make_async_remote_copy(
            far_out.at[c, f], far_in.at[c, f], far_send.at[c, f], far_recv.at[c, f],
            device_id={"tp": peer(cores + f)}, device_id_type=MESH)

    def far_return(c, f, j):
        at = pl.ds(j * block, block)
        return pltpu.make_async_remote_copy(
            far_res.at[c, f, :, at], far_back.at[c, f, :, at], far_rsend.at[c, f, j], far_rrecv.at[c, f, j],
            device_id={"tp": origin(cores + f)}, device_id_type=MESH)

    def near_copy(s):
        return pltpu.make_async_remote_copy(
            near_out.at[s], near_in.at[s], near_send.at[s], near_recv.at[s],
            device_id={"tp": peer(s)}, device_id_type=MESH)

    def near_return(s):
        return pltpu.make_async_remote_copy(
            near_res.at[s], near_back.at[s], near_rsend.at[s], near_rrecv.at[s],
            device_id={"tp": origin(s)}, device_id_type=MESH)

    for c in range(chunks):
        picks = jnp.concatenate([pick(cores + f, c * rows, rows) for f in range(far)], axis=0)
        if c == 0:
            loads[1].wait()
        far_out[c] = dot(picks, tokens[...]).astype(BF16).reshape(far, rows, width)
        if c == 0:
            pl.semaphore_wait(barrier, tp_count - 1)
        for f in range(far):
            far_copy(c, f).start()
    near_picks = jnp.concatenate([pick(s, 0, capacity) for s in range(cores)], axis=0)
    packed = dot(near_picks, tokens[...]).astype(BF16).reshape(cores, capacity, width)
    near_in[0] = packed[0]
    for s in range(1, cores):
        near_out[s] = packed[s]
        near_copy(s).start()

    for load in loads[2:5]:
        load.wait()
    gates = gates_ref[...]
    place = place_t.T
    gate_of = (jnp.where(first, gates[0:1, :], 0.0) + jnp.where(second, gates[1:2, :], 0.0)).T
    lane = lax.broadcasted_iota(jnp.int32, (tok_count, lanes), 1)

    def norm(load_rows, count):
        gain = gain_ref[...]
        bias = bias_ref[...]

        def norm_block(i, carry):
            at = pl.multiple_of(i * NORM_ROWS, NORM_ROWS)
            x = load_rows(at).astype(F32)
            center = jnp.mean(x, axis=-1, keepdims=True)
            centered = x - center
            variance = jnp.mean(centered * centered, axis=-1, keepdims=True)
            normed[pl.ds(at, NORM_ROWS), :] = (centered * lax.rsqrt(variance + EPSILON) * gain + bias).astype(BF16)
            return carry

        lax.fori_loop(0, count // NORM_ROWS, norm_block, 0)

    def hidden_of(count):
        rows_in = normed[pl.ds(0, count), :]
        gate_act = dot(rows_in, wg[...])
        up_act = dot(rows_in, wu[...])
        return (gate_act / (1.0 + jnp.exp(-gate_act)) * up_act).astype(BF16)

    for s in range(1, cores):
        near_copy(s).wait_recv()
    norm(lambda at: near_in[at // capacity, pl.ds(pl.multiple_of(at % capacity, NORM_ROWS), NORM_ROWS), :], cores * capacity)
    for load in loads[5:]:
        load.wait()
    results = dot(hidden_of(cores * capacity), wd[...]).astype(BF16).reshape(cores, capacity, width)
    near_back[0] = results[0]
    for s in range(1, cores):
        near_res[s] = results[s]
        near_return(s).start()

    def far_step(c, carry):
        for f in range(far):
            far_copy(c, f).wait_recv()
        norm(lambda at: far_in[c, at // rows, pl.ds(pl.multiple_of(at % rows, NORM_ROWS), NORM_ROWS), :], far * rows)
        hidden = hidden_of(far * rows)
        for j in range(BLOCKS):
            at = pl.ds(j * block, block)
            far_res[c, :, :, at] = dot(hidden, wd[:, at]).astype(BF16).reshape(far, rows, block)
            for f in range(far):
                far_return(c, f, j).start()
        return carry

    lax.fori_loop(0, chunks, far_step, 0)

    def spread(slots, start, count):
        want = lax.broadcasted_iota(jnp.int32, (tok_count, len(slots) * count), 1)
        high = jnp.zeros(want.shape, F32)
        for i, slot in enumerate(slots):
            mine = lane == peer(slot)
            at = jnp.sum(jnp.where(mine, place, 0.0), axis=1, keepdims=True).astype(jnp.int32) - start
            gate = jnp.sum(jnp.where(mine, gate_of, 0.0), axis=1, keepdims=True)
            at = jnp.where((at >= 0) & (at < count), at + i * count, -1)
            high = high + jnp.where(at == want, gate, 0.0)
        coarse = high.astype(BF16)
        return jnp.concatenate([coarse, (high - coarse.astype(F32)).astype(BF16)], axis=1)

    for s in range(1, cores):
        near_return(s).wait_recv()
    weights = spread(range(cores), 0, capacity)
    back = near_back[...].reshape(cores * capacity, width)
    total[...] = dot(weights, jnp.concatenate([back, back], axis=0))

    for c in range(chunks):
        weights = spread(range(cores, tp_count), c * rows, rows)
        for j in range(BLOCKS):
            at = pl.ds(j * block, block)
            for f in range(far):
                far_return(c, f, j).wait_recv()
            back = far_back[c, :, :, at].reshape(far * rows, block)
            part = total[:, at] + dot(weights, jnp.concatenate([back, back], axis=0))
            if c + 1 < chunks:
                total[:, at] = part
            else:
                out_ref[:, at] = part.astype(BF16)
    for s in range(1, cores):
        near_copy(s).wait_send()
        near_return(s).wait_send()

    def drain(c, carry):
        for f in range(far):
            far_copy(c, f).wait_send()
            for j in range(BLOCKS):
                far_return(c, f, j).wait_send()
        return carry

    lax.fori_loop(0, chunks, drain, 0)


def shards(token_rows, norm_gain, norm_bias, expert_ids, route_gates, gate_weight, up_weight, down_weight):
    tok_count, width = token_rows.shape
    hidden = gate_weight.shape[2]
    tp_count = lax.axis_size("tp")
    capacity = min(4 * tok_count // tp_count, tok_count // 2)
    cores = 2
    far = tp_count - cores
    chunks = max(1, capacity // CHUNK_ROWS)
    rows = capacity // chunks
    near = pltpu.VMEM((cores, capacity, width), BF16)
    distant = pltpu.VMEM((chunks, far, rows, width), BF16)
    near_sem = pltpu.SemaphoreType.DMA((cores,))
    far_sem = pltpu.SemaphoreType.DMA((chunks, far))
    ret_sem = pltpu.SemaphoreType.DMA((chunks, far, BLOCKS))
    return pl.pallas_call(
        functools.partial(kernel, tp_count, cores, capacity, chunks),
        out_shape=pltpu.VMEM((tok_count, width), BF16),
        in_specs=[pl.BlockSpec(memory_space=IN_SPACE)] * 8,
        out_specs=pl.BlockSpec(memory_space=pltpu.VMEM),
        scratch_shapes=[
            pltpu.VMEM((tok_count, width), BF16),
            pltpu.VMEM((1, width), F32),
            pltpu.VMEM((1, width), F32),
            pltpu.VMEM((2, tok_count), jnp.int32),
            pltpu.VMEM((2, tok_count), F32),
            pltpu.VMEM((width, hidden), BF16),
            pltpu.VMEM((width, hidden), BF16),
            pltpu.VMEM((hidden, width), BF16),
            pltpu.VMEM((max(cores * capacity, far * rows), width), BF16),
            near, near, near, near,
            distant, distant, distant, distant,
            pltpu.VMEM((tok_count, width), F32),
            pltpu.SemaphoreType.DMA((8,)),
            near_sem, near_sem, near_sem, near_sem,
            far_sem, far_sem, ret_sem, ret_sem,
        ],
        compiler_params=pltpu.CompilerParams(
            collective_id=0, has_side_effects=True, vmem_limit_bytes=VMEM_BYTES
        ),
    )(
        *(pltpu.with_memory_space_constraint(x, pltpu.HBM) for x in (
            token_rows, norm_gain.reshape(1, width), norm_bias.reshape(1, width),
            expert_ids.T, route_gates.T, gate_weight, up_weight, down_weight,
        ))
    )


def solution(mesh):
    rows = P(("grp", "ep", "tp"), None)
    weight = P("tp", None, None)
    return jax.shard_map(
        shards, mesh=mesh,
        in_specs=(rows, P(), P(), rows, rows, weight, weight, weight),
        out_specs=rows, check_vma=False,
    )
```
